32 devices in a mesh: sp: 8 (over z, y), tp: 4 (over x, core).
Axes of the slice: x: 2, y: 2, z: 4, core: 2. Of those that a mesh axis runs over, the one named last changes fastest.
Arguments:
- residual: bfloat16 [2048, 2048], P(('sp', 'tp')), may hold values from -6 to 6
- output_gate_projected: bfloat16 [2048, 4096], P('sp', 'tp'), may hold values from -6 to 6
- value_projected_input: bfloat16 [2048, 4096], P('sp', 'tp'), may hold values from -6 to 6
- state_projected_input: bfloat16 [2048, 2048], P('sp', 'tp'), may hold values from -6 to 6
- readout_projected_input: bfloat16 [2048, 2048], P('sp', 'tp'), may hold values from -6 to 6
- step_preactivation: float32 [2048, 64], P('sp', 'tp'), may hold values from -5 to 5
- position_decay_extra: float32 [2048, 64], P('sp', 'tp')
- value_conv_kernel: bfloat16 [4, 4096], P(None, 'tp'), may hold values from -0.29882812 to 0.29882812
- state_conv_kernel: bfloat16 [4, 2048], P(None, 'tp'), may hold values from -0.8984375 to 0.8984375
- readout_conv_kernel: bfloat16 [4, 2048], P(None, 'tp'), may hold values from -0.8984375 to 0.8984375
- head_log_decay_rates: float32 [64], P('tp')
- head_direct_weight: float32 [64], P('tp'), may hold values from 0.5 to 4
- head_norm_gain: float32 [4096], P('tp'), may hold values from 0.1 to 1.9
- mixer_output_weight: bfloat16 [4096, 2048], P('tp'), may hold values from -0.09375 to 0.09375
- expert_norm_gain: float32 [2048], replicated, may hold values from 0.1 to 1.9
- routed_expert_index: int32 [2048, 4], P(('sp', 'tp')), may hold values from 0 to 7, all different within a row; in each aligned block of 64 rows (0 to 63, 64 to 127, ...) at most 64 rows name the same one
- routed_expert_weight: float32 [2048, 4], P(('sp', 'tp')), may hold values from 0.2 to 1
- routed_gate_weight: bfloat16 [8, 2048, 256], P('sp'), may hold values from -0.125 to 0.125
- routed_up_weight: bfloat16 [8, 2048, 256], P('sp'), may hold values from -0.125 to 0.125
- routed_down_weight: bfloat16 [8, 256, 2048], P('sp'), may hold values from -0.375 to 0.375
- common_gate_weight: bfloat16 [2048, 512], P(None, 'tp'), may hold values from -0.125 to 0.125
- common_up_weight: bfloat16 [2048, 512], P(None, 'tp'), may hold values from -0.125 to 0.125
- common_down_weight: bfloat16 [2048, 512], P(None, 'tp'), may hold values from -0.25 to 0.25
Outputs:
- layer_out: bfloat16 [2048, 2048], P(('sp', 'tp'))
The draws below stay inside these ranges and needn't reach their ends.
Inputs may be any that keep to these rules, and one draw needn't show every extreme that they name: `routed_expert_index`: among the 64 rows of one device, no expert is named by more than 64 rows.
All inputs are finite; a program needn't handle non-finite values.
Results may differ from the reference program's by a relative error of at most 0.02.
Values may be sent and summed in bfloat16 or wider, within the bound.
No kernel may reach another device: no remote copies, remote signals or barrier semaphores. Data moves between devices by JAX's collectives and lax.ppermute only.
A program may use at most 128 MiB of HBM per device.

```python
import math
import jax
import jax.numpy as jnp
import numpy as np
from jax import lax

D = 2048
HEAD_DIM = 64
HEADS = 64
HEAD_GROUPS = 16
STATE = 128
CONV = 4
BLOCK_POSITIONS = 128
FE = 256
FS = 512
TOPK = 4
TOK_DEV = 256
INNER = 4096
SEQ = 2048
ROWS = 64
EXPERTS = 8
CAP = 64
N_TP = 4


def draw_step_preactivation(key, part):
    base_key, shift_key = jax.random.split(jax.random.fold_in(key, 11))
    block_list = SEQ // TOK_DEV
    jitter = jnp.clip(jax.random.normal(base_key, (SEQ, HEADS), jnp.float32), -4.0, 4.0)
    offsets = jax.random.uniform(shift_key, (block_list, 1, HEADS), jnp.float32, -1.0, 1.0)
    return (jitter.reshape(block_list, TOK_DEV, HEADS) + offsets).reshape(SEQ, HEADS)


def draw_head_log_decay_rates(key, part):
    pick_key, fast_key, slow_key = jax.random.split(jax.random.fold_in(key, 23), 3)
    ranking = jax.random.permutation(pick_key, HEADS)
    fast = ranking < HEADS // 2
    fast_rate = jax.random.uniform(fast_key, (HEADS,), jnp.float32, math.log(2.0 / BLOCK_POSITIONS), math.log(6.0 / BLOCK_POSITIONS))
    slow_rate = jax.random.uniform(slow_key, (HEADS,), jnp.float32, math.log(0.1 / SEQ), math.log(0.6 / SEQ))
    return jnp.where(fast, fast_rate, slow_rate)


def draw_position_decay_extra(key, part):
    place_key, depth_key = jax.random.split(jax.random.fold_in(key, 37))
    places = jax.random.randint(place_key, (3,), 0, SEQ)
    depths = jax.random.uniform(depth_key, (3, HEADS), jnp.float32, math.log(0.6), math.log(0.8))
    return jnp.zeros((SEQ, HEADS), jnp.float32).at[places].add(depths)


def steps_of(rng, dims, pieces, least, high):
    def one(position, parts):
        heights = jax.random.uniform(jax.random.fold_in(jax.random.fold_in(rng, 6), position), (parts,), jnp.float32, least / len(pieces), high / len(pieces))
        return jnp.repeat(jnp.exp(heights), dims[position] // parts).reshape((-1,) + (1,) * (len(dims) - position - 1))

    loudness = one(*pieces[0])
    for cut in pieces[1:]:
        loudness = loudness * one(*cut)
    return loudness


def assign_block(own_key, own, number, rows, count, top, bound, slope):
    sequence = jax.random.permutation(own_key, count)
    packed, common = load_shares(count, rows * top, bound, slope, True), load_shares(count, rows * top, bound, slope, False)
    places = jnp.arange(count)

    def named(tallies, turn):
        used = int((tallies > 0).sum())
        fixed = max(1, used // 4)
        moved = fixed + (places - fixed + turn * (used - fixed)) % max(1, count - fixed)
        return jnp.zeros((count,), jnp.int32).at[sequence[jnp.where(places < fixed, places, moved)]].set(jnp.asarray(tallies, jnp.int32))

    tallies = jnp.where(number % 4 == 0, named(packed, number // 4), named(common, number - number // 4 - 1))
    mixed = jax.random.permutation(jax.random.fold_in(own, 3), count)
    source_of, sink = mixed[0:count // 2 * 2:2], mixed[1:count // 2 * 2:2]
    slack = jnp.minimum(tallies[source_of] - 1, bound - tallies[sink]) // 2
    slack = jnp.where((source_of == sequence[0]) | (sink == sequence[0]) | (tallies[sink] == 0), 0, jnp.maximum(slack, 0))
    moved = jax.random.randint(jax.random.fold_in(own, 4), (count // 2,), 0, 1 << 20) % (slack + 1)
    tallies = tallies.at[source_of].add(-moved).at[sink].add(moved)
    members = jnp.searchsorted(jnp.cumsum(tallies), jnp.arange(rows * top), side="right").astype(jnp.int32)
    table = members.reshape(top, rows).T
    table = table[jax.random.permutation(jax.random.fold_in(own, 1), rows)]
    turn = jax.random.randint(jax.random.fold_in(own, 2), (rows, 1), 0, top)
    return jnp.take_along_axis(table, (jnp.arange(top)[None, :] + turn) % top, axis=1)


def load_shares(number_of, total, reach, lean, full):
    portions = [(1 << 20) // math.isqrt(grade ** lean) + 1 for grade in range(1, number_of + 1)]
    largest = reach if full else min(reach, max(-(-total // number_of), total * portions[0] // sum(portions)))
    least = 1 if total - largest >= number_of - 1 else 0
    holding, surplus = [largest] + [least] * (number_of - 1), total - largest - least * (number_of - 1)
    while surplus > 0:
        candidates = [i for i in range(1, number_of) if holding[i] < largest] or [i for i in range(1, number_of) if holding[i] < reach]
        mass, remaining = sum([portions[i] for i in candidates]), surplus
        for i in candidates:
            more = min(reach - holding[i], max(1, remaining * portions[i] // mass), surplus)
            holding[i] = holding[i] + more
            surplus = surplus - more
    return np.array(holding)


def scatter_about(rng, dims, deviation, most, pieces=(), held_as=jnp.bfloat16):
    values = deviation * jax.random.normal(rng, dims, jnp.float32)
    if pieces:
        values = values * steps_of(rng, dims, pieces, -0.22, 0.18)
    return jnp.clip(values, -most, most).astype(held_as)


def setup_inputs(seed: int = 0) -> dict:
    arg_keys = jax.random.split(jax.random.key(seed), 24)
    residual = scatter_about(arg_keys[0], (SEQ, D), 1.0, 6.0, ((0, 32),))
    output_gate_projected = scatter_about(arg_keys[1], (SEQ, INNER), 1.0, 6.0, ((0, 8), (1, 4)))
    value_projected_input = scatter_about(arg_keys[2], (SEQ, INNER), 1.0, 6.0, ((0, 8), (1, 4)))
    state_projected_input = scatter_about(arg_keys[3], (SEQ, HEAD_GROUPS * STATE), 1.0, 6.0, ((0, 8), (1, 4)))
    readout_projected_input = scatter_about(arg_keys[4], (SEQ, HEAD_GROUPS * STATE), 1.0, 6.0, ((0, 8), (1, 4)))
    step_preactivation = draw_step_preactivation(jax.random.fold_in(arg_keys[23], 71), 0)
    position_decay_extra = draw_position_decay_extra(jax.random.fold_in(arg_keys[23], 71), 0)
    value_conv_kernel = scatter_about(arg_keys[7], (CONV, INNER), 0.05, 0.29882812, ((1, 4),))
    state_conv_kernel = scatter_about(arg_keys[8], (CONV, HEAD_GROUPS * STATE), 0.15, 0.8984375, ((1, 4),))
    readout_conv_kernel = scatter_about(arg_keys[9], (CONV, HEAD_GROUPS * STATE), 0.15, 0.8984375, ((1, 4),))
    head_log_decay_rates = draw_head_log_decay_rates(jax.random.fold_in(arg_keys[23], 71), 0)
    head_direct_weight = jnp.clip(jnp.exp(math.log(4.0) - 2.0794415 * jax.random.uniform(arg_keys[11], (HEADS,), jnp.float32) ** steps_of(arg_keys[11], (HEADS,), ((0, 4),), -0.2, 0.2)), 0.5, 4.0)
    head_norm_gain = jnp.clip(1.0 + 0.18 * jax.random.normal(arg_keys[12], (INNER,), jnp.float32), 0.1, 1.9)
    mixer_output_weight = scatter_about(arg_keys[13], (INNER, D), INNER ** -0.5, 0.09375, ((0, 4),))
    expert_norm_gain = jnp.clip(1.0 + 0.18 * jax.random.normal(arg_keys[14], (D,), jnp.float32), 0.1, 1.9)
    routed_expert_index_keys = jax.random.split(jax.random.fold_in(arg_keys[15], 1), SEQ // ROWS)
    routed_expert_index_turns = jax.random.permutation(jax.random.fold_in(arg_keys[15], 3), SEQ // ROWS)
    routed_expert_index = jax.vmap(lambda own, number: assign_block(jax.random.fold_in(arg_keys[15], 2), own, number, ROWS, EXPERTS, TOPK, CAP, 2))(routed_expert_index_keys, routed_expert_index_turns).reshape((SEQ, TOPK))
    routed_expert_weight = jnp.clip(0.2 + 0.8 * jax.random.uniform(arg_keys[16], (SEQ, TOPK), jnp.float32) ** steps_of(arg_keys[16], (SEQ, TOPK), ((0, 32),), -0.2, 0.2), 0.2, 1.0)
    routed_gate_weight = scatter_about(arg_keys[17], (EXPERTS, D, FE), D ** -0.5, 0.125, ((0, 8),))
    routed_up_weight = scatter_about(arg_keys[18], (EXPERTS, D, FE), D ** -0.5, 0.125, ((0, 8),))
    routed_down_weight = scatter_about(arg_keys[19], (EXPERTS, FE, D), FE ** -0.5, 0.375, ((0, 8),))
    common_gate_weight = scatter_about(arg_keys[20], (D, FS), D ** -0.5, 0.125, ((1, 4),))
    common_up_weight = scatter_about(arg_keys[21], (D, FS), D ** -0.5, 0.125, ((1, 4),))
    common_down_weight = scatter_about(arg_keys[22], (D, FS), FS ** -0.5, 0.25, ((1, 4),))
    return dict(residual=residual, output_gate_projected=output_gate_projected, value_projected_input=value_projected_input, state_projected_input=state_projected_input, readout_projected_input=readout_projected_input, step_preactivation=step_preactivation, position_decay_extra=position_decay_extra, value_conv_kernel=value_conv_kernel, state_conv_kernel=state_conv_kernel, readout_conv_kernel=readout_conv_kernel, head_log_decay_rates=head_log_decay_rates, head_direct_weight=head_direct_weight, head_norm_gain=head_norm_gain, mixer_output_weight=mixer_output_weight, expert_norm_gain=expert_norm_gain, routed_expert_index=routed_expert_index, routed_expert_weight=routed_expert_weight, routed_gate_weight=routed_gate_weight, routed_up_weight=routed_up_weight, routed_down_weight=routed_down_weight, common_gate_weight=common_gate_weight, common_up_weight=common_up_weight, common_down_weight=common_down_weight)


EPSILON = 1e-06
HIGHEST_PRECISION = lax.Precision.HIGHEST

def short_conv(inputs, weights):
    length = inputs.shape[0]
    padded = jnp.pad(inputs.astype(jnp.float32), ((CONV - 1, 0), (0, 0)))
    totals = jnp.zeros((length, inputs.shape[1]), jnp.float32)
    for tap_index in range(CONV):
        totals = totals + padded[tap_index:tap_index + length] * weights[tap_index].astype(jnp.float32)
    return jax.nn.silu(totals)

def swiglu_rows(rows, gate_weight, up_weight, down_weight):
    gate_part = jnp.dot(rows, gate_weight, preferred_element_type=jnp.float32)
    lifted = jnp.dot(rows, up_weight, preferred_element_type=jnp.float32)
    hidden = (jax.nn.silu(gate_part) * lifted).astype(jnp.bfloat16)
    return jnp.dot(hidden, down_weight, preferred_element_type=jnp.float32)

def reference(residual, output_gate_projected, value_projected_input, state_projected_input, readout_projected_input, step_preactivation, position_decay_extra, value_conv_kernel, state_conv_kernel, readout_conv_kernel, head_log_decay_rates, head_direct_weight, head_norm_gain, mixer_output_weight, expert_norm_gain, routed_expert_index, routed_expert_weight, routed_gate_weight, routed_up_weight, routed_down_weight, common_gate_weight, common_up_weight, common_down_weight):
    heads_per_group = HEADS // HEAD_GROUPS
    block_list = SEQ // BLOCK_POSITIONS
    values = short_conv(value_projected_input, value_conv_kernel).reshape(block_list, BLOCK_POSITIONS, HEAD_GROUPS, heads_per_group, HEAD_DIM)
    state_in = short_conv(state_projected_input, state_conv_kernel).reshape(block_list, BLOCK_POSITIONS, HEAD_GROUPS, STATE)
    readout = short_conv(readout_projected_input, readout_conv_kernel).reshape(block_list, BLOCK_POSITIONS, HEAD_GROUPS, STATE)
    head_step_lengths = jax.nn.softplus(step_preactivation)
    decay_logarithm = (head_step_lengths * (-jnp.exp(head_log_decay_rates))[None, :] + position_decay_extra).reshape(block_list, BLOCK_POSITIONS, HEAD_GROUPS, heads_per_group)
    head_step_lengths = head_step_lengths.reshape(block_list, BLOCK_POSITIONS, HEAD_GROUPS, heads_per_group)
    gates = output_gate_projected.reshape(block_list, BLOCK_POSITIONS, HEADS, HEAD_DIM)
    streams = residual.reshape(block_list, BLOCK_POSITIONS, D)
    skips = head_direct_weight.reshape(HEAD_GROUPS, heads_per_group)
    gains = head_norm_gain.reshape(HEADS, HEAD_DIM)
    out_parts = mixer_output_weight.astype(jnp.float32).reshape(N_TP, INNER // N_TP, D)
    causal = jnp.arange(BLOCK_POSITIONS)[:, None] >= jnp.arange(BLOCK_POSITIONS)[None, :]

    def block_step(carried, block_inputs):
        value_blk, input_blk, readout_blk, decay_blk, sizes_blk, gate_blk, stream_blk = block_inputs
        cumulative = jnp.cumsum(decay_blk, axis=0)
        weighted_output = value_blk * sizes_blk[..., None]
        by_head = jnp.transpose(cumulative, (1, 2, 0))
        span_logs = by_head[:, :, :, None] - by_head[:, :, None, :]
        decay_factors = jnp.exp(jnp.where(causal, span_logs, -jnp.inf))
        attention_scores = jnp.einsum('tgn,sgn->gts', readout_blk, input_blk, precision=HIGHEST_PRECISION)
        within_block_output = jnp.einsum('wkij,jwke->iwke', attention_scores[:, None] * decay_factors, weighted_output, precision=HIGHEST_PRECISION)
        carried_out = jnp.einsum('tgn,grpn->tgrp', readout_blk, carried, precision=HIGHEST_PRECISION) * jnp.exp(cumulative)[..., None]
        mixed_heads = within_block_output + carried_out + skips[None, :, :, None] * value_blk
        to_end = jnp.exp(cumulative[-1:] - cumulative)
        fresh_state = jnp.einsum('sgn,sgrp->grpn', input_blk, weighted_output * to_end[..., None], precision=HIGHEST_PRECISION)
        carried = jnp.exp(cumulative[-1])[..., None, None] * carried + fresh_state
        mixed_heads = mixed_heads.reshape(BLOCK_POSITIONS, HEADS, HEAD_DIM) * jax.nn.silu(gate_blk.astype(jnp.float32))
        normed = mixed_heads * lax.rsqrt(lax.optimization_barrier(jnp.mean(mixed_heads * mixed_heads, axis=-1, keepdims=True)) + EPSILON) * gains
        heads_out = lax.optimization_barrier(normed.astype(jnp.bfloat16)).astype(jnp.float32)
        heads_out = heads_out.reshape(BLOCK_POSITIONS, N_TP, INNER // N_TP)
        partials = jnp.einsum('tqi,qid->qtd', heads_out, out_parts).astype(jnp.bfloat16)
        partials = lax.optimization_barrier(partials).astype(jnp.float32)
        stream = stream_blk.astype(jnp.float32) + lax.optimization_barrier(jnp.sum(partials, axis=0))
        return (carried, stream.astype(jnp.bfloat16))
    start_state = jnp.zeros((HEAD_GROUPS, heads_per_group, HEAD_DIM, STATE), jnp.float32)
    _, stream = lax.scan(block_step, start_state, (values, state_in, readout, decay_logarithm, head_step_lengths, gates, streams))
    stream = stream.reshape(SEQ, D).astype(jnp.float32)
    normed_rows = (stream * lax.rsqrt(lax.optimization_barrier(jnp.mean(stream * stream, axis=-1, keepdims=True)) + EPSILON) * expert_norm_gain).astype(jnp.bfloat16)
    shared = swiglu_rows(normed_rows, common_gate_weight, common_up_weight, common_down_weight.T)
    group_rows = 128
    tokens = SEQ
    assignments = tokens * TOPK
    flat_ids = routed_expert_index.reshape(-1).astype(jnp.int32)
    sort_order = jnp.argsort(flat_ids).astype(jnp.int32)
    sorted_ids = flat_ids[sort_order]
    counts = lax.optimization_barrier(jnp.sum((flat_ids[:, None] == jnp.arange(EXPERTS, dtype=jnp.int32)[None, :]).astype(jnp.int32), axis=0)).astype(jnp.int32)
    padded = ((counts + group_rows - 1) // group_rows * group_rows).astype(jnp.int32)
    starts = (jnp.cumsum(counts) - counts).astype(jnp.int32)
    pad_end = jnp.cumsum(padded).astype(jnp.int32)
    pad_start = (pad_end - padded).astype(jnp.int32)
    destination = (pad_start[sorted_ids] + jnp.arange(assignments, dtype=jnp.int32) - starts[sorted_ids]).astype(jnp.int32)
    nblocks = -(-assignments // group_rows) + EXPERTS
    rows_total = nblocks * group_rows
    row_token = jnp.full((rows_total,), tokens, jnp.int32).at[destination].set((sort_order // TOPK).astype(jnp.int32))
    row_weight = jnp.zeros((rows_total,), jnp.float32).at[destination].set(routed_expert_weight.reshape(-1)[sort_order])
    block_expert = jnp.minimum(jnp.searchsorted(pad_end, jnp.arange(nblocks, dtype=jnp.int32) * group_rows, side='right'), EXPERTS - 1).astype(jnp.int32)
    padded_rows = jnp.concatenate([normed_rows, jnp.zeros((1, D), jnp.bfloat16)], axis=0)

    def expert_block(block_args):
        token_ids, expert_id = block_args
        chosen = padded_rows[token_ids]
        return swiglu_rows(chosen, routed_gate_weight[expert_id], routed_up_weight[expert_id], routed_down_weight[expert_id]).astype(jnp.bfloat16)
    outputs = lax.map(expert_block, (row_token.reshape(nblocks, group_rows), block_expert))
    contrib = outputs.reshape(rows_total, D).astype(jnp.float32) * row_weight[:, None]
    routed = jnp.zeros((tokens + 1, D), jnp.float32).at[row_token].add(contrib)[:tokens]
    return (stream + shared + routed).astype(jnp.bfloat16)
```

```python
import functools

import jax
import jax.numpy as jnp
from jax import lax
from jax.experimental import pallas as pl
from jax.experimental.pallas import tpu as pltpu
from jax.sharding import PartitionSpec as P

HEAD_DIM = 64
STATE = 128
CONV = 4
BLOCK = 128
LANES = 128
RIM = 8
PAD_ROWS = 16
EPSILON = 1e-06

F32 = jnp.float32
BF16 = jnp.bfloat16


def dot(a, b):
    return jnp.dot(a, b, preferred_element_type=F32)


def silu(t):
    half = 0.5 * t
    return half + half * jnp.tanh(half)


def call(kernel, outs, *args, flops=0, scratch=(), specs=None):
    out_shape = [jax.ShapeDtypeStruct(s, d) for s, d in outs]
    nbytes = sum(a.size * a.dtype.itemsize for a in args)
    if specs is None:
        specs = [None] * len(args)
    whole = pl.BlockSpec(memory_space=pltpu.VMEM)
    return pl.pallas_call(
        kernel,
        out_shape=out_shape,
        in_specs=[whole if s is None else s for s in specs],
        out_specs=[whole] * len(outs),
        scratch_shapes=list(scratch),
        cost_estimate=pl.CostEstimate(flops=flops, transcendentals=0, bytes_accessed=nbytes),
        compiler_params=pltpu.CompilerParams(vmem_limit_bytes=56 * 1024 * 1024),
    )(*args)


SMEM = pl.BlockSpec(memory_space=pltpu.SMEM)
HBM = pl.BlockSpec(memory_space=pl.ANY)


def head_expander(heads):
    width = heads * HEAD_DIM
    row = lax.broadcasted_iota(jnp.int32, (heads, width), 0)
    col = lax.broadcasted_iota(jnp.int32, (heads, width), 1) // HEAD_DIM
    return (row == col).astype(F32).astype(BF16)


def expand(per_head, expander):
    high = per_head.astype(BF16)
    low = (per_head - high.astype(F32)).astype(BF16)
    return dot(high, expander) + dot(low, expander)


def conv_slab(ext, current, before, taps):
    rows = current.shape[0]
    ext[0:RIM, :] = before.astype(F32)
    ext[RIM : RIM + rows, :] = current.astype(F32)
    total = ext[RIM - CONV + 1 : RIM - CONV + 1 + rows, :] * taps[0:1, :]
    for k in range(1, CONV):
        begin = RIM - CONV + 1 + k
        total = total + ext[begin : begin + rows, :] * taps[k : k + 1, :]
    return silu(total)


def front_kernel(block, groups, *refs):
    (x, bmat, step, extra, rates, wx, wb) = refs[:7]
    if block == 0:
        rim, f_late, dec_late = refs[7:10]
        val, bout, dt_out, cum_out, f_out, chunks = refs[10:16]
        ext, ext_b = refs[16:18]
    else:
        val, bout, dt_out, cum_out, f_out, dec_out = refs[7:13]
        ext, ext_b = refs[13:15]
    lo = block * BLOCK
    heads = step.shape[1]
    inner = x.shape[1]
    group_width = inner // groups
    rows = slice(lo, lo + BLOCK)
    pre = step[rows, :]
    dt = jnp.maximum(pre, 0.0) + jnp.log1p(jnp.exp(-jnp.abs(pre)))
    decay = dt * (-jnp.exp(rates[0:1, :])) + extra[rows, :]
    r = lax.broadcasted_iota(jnp.int32, (BLOCK, BLOCK), 0)
    c = lax.broadcasted_iota(jnp.int32, (BLOCK, BLOCK), 1)
    tri = (r >= c).astype(F32)
    cum = jnp.dot(tri, decay, precision=lax.Precision.HIGHEST, preferred_element_type=F32)
    dt_out[...] = dt
    cum_out[...] = cum
    last = cum[BLOCK - 1 : BLOCK, :]
    expander = head_expander(heads)
    weight = expand(dt * jnp.exp(last - cum), expander)
    total = expand(jnp.broadcast_to(jnp.exp(last), (8, heads)), expander)
    for g in range(groups):
        xl = slice(g * group_width, (g + 1) * group_width)
        bl = slice(g * STATE, (g + 1) * STATE)
        if block == 0:
            before_x = rim[:, xl]
            before_b = rim[:, inner + g * STATE : inner + (g + 1) * STATE]
        else:
            before_x = x[lo - RIM : lo, xl]
            before_b = bmat[lo - RIM : lo, bl]
        v = conv_slab(ext, x[rows, xl], before_x, wx[:, xl].astype(F32))
        val[:, xl] = v.astype(BF16)
        bs = conv_slab(ext_b, bmat[rows, bl], before_b, wb[:, bl].astype(F32)).astype(BF16)
        bout[:, bl] = bs
        xw = (v * weight[:, xl]).astype(BF16)
        fresh = lax.dot_general(bs, xw, (((0,), (0,)), ((), ())), preferred_element_type=F32)
        gr = slice(g * STATE, (g + 1) * STATE)
        f_out[gr, :] = fresh.astype(f_out.dtype)
        if block == 0:
            own = fresh * dec_late[0:1, xl] + f_late[gr, :]
            both = total[:, xl] * dec_late[:, xl]
            per = chunks.shape[1] - PAD_ROWS
            pad_row = lax.broadcasted_iota(jnp.int32, (PAD_ROWS, LANES), 0)
            for s in range(group_width // LANES):
                sl = slice(s * LANES, (s + 1) * LANES)
                dec = jnp.concatenate([both[:, sl]] * (PAD_ROWS // 8), axis=0)
                high = dec.astype(BF16).astype(F32)
                tail = jnp.where(pad_row == 0, high, jnp.where(pad_row == 1, dec - high, 0.0))
                for part in range(STATE // per):
                    index = ((g * (group_width // LANES) + s) * STATE) // per + part
                    chunks[index, 0:per, :] = own[part * per : (part + 1) * per, sl].astype(BF16)
                    chunks[index, per : per + PAD_ROWS, :] = tail.astype(BF16)
        else:
            dec_out[:, xl] = total[:, xl]


def scan_kernel(arrived, out):
    count = arrived.shape[0]
    per = out.shape[1]

    def hop(j, state):
        out[j] = state.astype(BF16)
        piece = arrived[j]
        decay = piece[per : per + 1].astype(F32) + piece[per + 1 : per + 2].astype(F32)
        return state * decay + piece[0:per].astype(F32)

    lax.fori_loop(0, count, hop, jnp.zeros(out.shape[1:], F32))


def middle_kernel(groups, *refs):
    (cmat, rim, wc, gate, direct) = refs[:5]
    vals, bs, dts, cums = refs[5:7], refs[7:9], refs[9:11], refs[11:13]
    first_state = refs[13]
    y_out, c_out, g_out, e_out, ext = refs[14:19]
    heads = dts[0].shape[1]
    inner = gate.shape[1]
    group_width = inner // groups
    slabs = group_width // LANES
    expander = head_expander(heads)
    skip = expand(jnp.broadcast_to(direct[0:1, :], (8, heads)), expander)
    r = lax.broadcasted_iota(jnp.int32, (BLOCK, BLOCK), 0)
    c = lax.broadcasted_iota(jnp.int32, (BLOCK, BLOCK), 1)
    causal = r >= c
    lane = lax.broadcasted_iota(jnp.int32, (BLOCK, LANES), 1)
    low_head = lane < HEAD_DIM
    zero = jnp.zeros((BLOCK, LANES), F32)
    before_total = None
    for b in range(2):
        rows = slice(b * BLOCK, (b + 1) * BLOCK)
        cum = cums[b][...]
        cum_t = jnp.concatenate([cum, jnp.zeros((BLOCK, LANES - heads), F32)], axis=1).T
        dt_x = expand(dts[b][...], expander)
        own_decay = jnp.exp(cum)
        own_x = expand(own_decay, expander)
        if b == 0:
            e_out[rows, :] = own_x.astype(BF16)
            before_total = cum[BLOCK - 1 : BLOCK, :]
        else:
            e_out[rows, :] = expand(jnp.exp(cum + before_total), expander).astype(BF16)
        for g in range(groups):
            cl = slice(g * STATE, (g + 1) * STATE)
            before = rim[:, inner + groups * STATE + g * STATE : inner + groups * STATE + (g + 1) * STATE] if b == 0 else cmat[BLOCK - RIM : BLOCK, cl]
            cs = conv_slab(ext, cmat[rows, cl], before, wc[:, cl].astype(F32)).astype(BF16)
            c_out[rows, cl] = cs
            bsg = bs[b][:, cl]
            scores = lax.dot_general(cs, bsg, (((1,), (1,)), ((), ())), preferred_element_type=F32)
            for s in range(slabs):
                first = g * group_width + s * LANES
                sl = slice(first, first + LANES)
                h = first // HEAD_DIM
                value = vals[b][:, sl].astype(F32)
                xw = value * dt_x[:, sl]
                mats = []
                for k in range(2):
                    span = cum[:, h + k : h + k + 1] - cum_t[h + k : h + k + 1, :]
                    mats.append((scores * jnp.exp(jnp.where(causal, span, -jnp.inf))).astype(BF16))
                left = jnp.concatenate(mats, axis=1)
                right = jnp.concatenate(
                    [jnp.where(low_head, xw, zero).astype(BF16), jnp.where(low_head, zero, xw).astype(BF16)],
                    axis=0,
                )
                y = dot(left, right) + skip[0:1, sl] * value
                if b == 1:
                    y = y + own_x[:, sl] * dot(cs, first_state[g * STATE : (g + 1) * STATE, s * LANES : (s + 1) * LANES])
                y_out[rows, sl] = y
                g_out[rows, sl] = silu(gate[rows, sl].astype(F32)).astype(BF16)


def mixer_kernel(groups, tp_size, *refs):
    (place, states, y_in, c_in, g_in, e_in, gain, weight) = refs[:8]
    outs = refs[8 : 8 + tp_size]
    heads_out, part, wbuf, sems = refs[8 + tp_size :]
    inner, width = weight.shape
    chunk_count = wbuf.shape[0]
    chunk = width // chunk_count
    copies = [
        pltpu.make_async_copy(weight.at[:, pl.ds(n * chunk, chunk)], wbuf.at[n], sems.at[n])
        for n in range(chunk_count)
    ]
    for copy in copies:
        copy.start()
    row = lax.broadcasted_iota(jnp.int32, (LANES, LANES), 0) // HEAD_DIM
    col = lax.broadcasted_iota(jnp.int32, (LANES, LANES), 1) // HEAD_DIM
    same = jnp.where(row == col, 1.0 / HEAD_DIM, 0.0).astype(BF16)
    slabs = inner // groups // LANES
    for e in range(inner // LANES):
        g = e // slabs
        sl = slice(e * LANES, (e + 1) * LANES)
        carried = dot(c_in[:, g * STATE : (g + 1) * STATE], states[e * STATE : (e + 1) * STATE, :])
        y = (y_in[:, sl] + carried * e_in[:, sl].astype(F32)) * g_in[:, sl].astype(F32)
        square = y * y
        high = square.astype(BF16)
        low = (square - high.astype(F32)).astype(BF16)
        mean = dot(high, same) + dot(low, same)
        heads_out[:, sl] = (y * lax.rsqrt(mean + EPSILON) * gain[0:1, sl]).astype(BF16)
    everything = heads_out[...]
    for n in range(chunk_count):
        copies[n].wait()
        part[:, n * chunk : (n + 1) * chunk] = dot(everything, wbuf[n]).astype(BF16)
    count = outs[0].shape[0]
    for k in range(tp_size):
        begin = pl.multiple_of((place[0] ^ k) * count, count)
        outs[k][...] = part[pl.ds(begin, count), :]


def stream_kernel(*refs):
    residual, gain = refs[:2]
    parts = refs[2:-2]
    stream_out, rows_out = refs[-2:]
    total = parts[0][...].astype(F32)
    for part in parts[1:]:
        total = total + part[...].astype(F32)
    stream = (residual[...].astype(F32) + total).astype(BF16)
    stream_out[...] = stream
    wide = stream.astype(F32)
    mean = jnp.mean(wide * wide, axis=-1, keepdims=True)
    rows_out[...] = (wide * lax.rsqrt(mean + EPSILON) * gain[0:1, :]).astype(BF16)


def shared_kernel(*refs):
    rows_ref, stream_ref = refs[:2]
    weights = refs[2:-1]
    out = refs[-1]
    rows = rows_ref[...]
    total = stream_ref[...].astype(F32)
    count = len(weights) // 2
    for k in range(count):
        both = dot(rows, weights[k][...])
        half = both.shape[1] // 2
        hidden = (silu(both[:, :half]) * both[:, half:]).astype(BF16)
        total = total + lax.dot_general(
            hidden, weights[count + k][...], (((1,), (1,)), ((), ())), preferred_element_type=F32
        )
    out[...] = total


def expert_kernel(slot_parts, *refs):
    place = refs[0]
    total_in = sum(slot_parts)
    inputs = refs[1 : 1 + total_in]
    tables = refs[1 + total_in : 1 + 2 * total_in]
    wg, wu, wd, gu_a, gu_b, d_a, d_b = refs[1 + 2 * total_in : 8 + 2 * total_in]
    outs = refs[8 + 2 * total_in :]
    blocks, weights, at = [], [], 0
    for parts in slot_parts:
        block, table = inputs[at][...], tables[at][...]
        for k in range(1, parts):
            block = block + inputs[at + k][...]
            table = table + tables[at + k][...]
        blocks.append(block)
        weights.append(table)
        at += parts
    rows = jnp.concatenate(blocks, axis=0)
    table = jnp.concatenate(weights, axis=0)
    lane = lax.broadcasted_iota(jnp.int32, table.shape, 1)
    own = jnp.sum(jnp.where(lane == place[0], table, 0.0), axis=1, keepdims=True)
    other = jnp.sum(jnp.where(lane == (place[0] ^ 1), table, 0.0), axis=1, keepdims=True)
    hidden = (silu(dot(rows, wg[0])) * dot(rows, wu[0]) * own).astype(BF16)
    total = dot(hidden, wd[0])
    for gu, down in ((gu_a, d_a), (gu_b, d_b)):
        both = dot(rows, gu[...])
        half = both.shape[1] // 2
        hidden = (silu(both[:, :half]) * both[:, half:] * other).astype(BF16)
        total = total + dot(hidden, down[...])
    count = outs[0].shape[0]
    for k, out in enumerate(outs):
        out[...] = total[k * count : (k + 1) * count].astype(BF16)


def plain_shared(rows, gate_piece, up_piece, down_piece):
    gate_part = jnp.dot(rows, gate_piece, preferred_element_type=F32)
    lifted = jnp.dot(rows, up_piece, preferred_element_type=F32)
    hidden = (jax.nn.silu(gate_part) * lifted).astype(BF16)
    return jnp.einsum("rc,dc->rd", hidden, down_piece, preferred_element_type=F32)


def sparse_experts(stream, normed_rows, index, weights, wg, wu, wd, cg, cu, cd):
    width = stream.shape[1]
    row_count, top_count = index.shape
    group_rows = lax.all_gather(normed_rows, "tp", axis=0, tiled=True)
    shared = lax.psum_scatter(
        plain_shared(group_rows, cg, cu, cd).astype(BF16), "tp", scatter_dimension=0, tiled=True
    ).astype(F32)
    local_experts = wg.shape[0]
    experts_all = local_experts * lax.axis_size("sp")
    capacity = min(row_count, 2 * row_count * top_count // experts_all)
    flat_ids = index.reshape(-1)
    hits = (flat_ids[:, None] == jnp.arange(experts_all, dtype=jnp.int32)[None, :]).astype(jnp.int32)
    ranks = jnp.sum((jnp.cumsum(hits, axis=0) - 1) * hits, axis=1)
    slot_index = flat_ids * capacity + ranks
    slot_rows = (
        jnp.full((experts_all * capacity,), row_count, jnp.int32)
        .at[slot_index]
        .set(jnp.arange(row_count * top_count, dtype=jnp.int32) // top_count)
    )
    padded = jnp.concatenate([normed_rows, jnp.zeros((1, width), BF16)], axis=0)
    outgoing = padded[slot_rows].reshape(experts_all, capacity, width)
    arrived = lax.all_to_all(outgoing, "sp", split_axis=0, concat_axis=0, tiled=True)
    sources = arrived.shape[0] // local_experts
    grouped = arrived.reshape(sources, local_experts, arrived.shape[1], width)
    gate_part = jnp.einsum("sekd,edf->sekf", grouped, wg, preferred_element_type=F32)
    lifted = jnp.einsum("sekd,edf->sekf", grouped, wu, preferred_element_type=F32)
    hidden = (jax.nn.silu(gate_part) * lifted).astype(BF16)
    result = jnp.einsum("sekf,efd->sekd", hidden, wd, preferred_element_type=F32).astype(BF16)
    returned = lax.all_to_all(
        result.reshape(arrived.shape), "sp", split_axis=0, concat_axis=0, tiled=True
    )
    picked = returned.reshape(experts_all * capacity, width)[slot_index]
    routed = jnp.sum(
        (picked.astype(F32) * weights.reshape(-1)[:, None]).reshape(row_count, top_count, width),
        axis=1,
    )
    return (stream.astype(F32) + shared + routed).astype(BF16)


def line_pairs(line, moves):
    return [(2 * a + y, 2 * b + y) for a, b in moves for y in range(2) if 0 <= a < line and 0 <= b < line]


def shards(
    residual,
    output_gate_projected,
    value_projected_input,
    state_projected_input,
    readout_projected_input,
    step_preactivation,
    position_decay_extra,
    value_conv_kernel,
    state_conv_kernel,
    readout_conv_kernel,
    head_log_decay_rates,
    head_direct_weight,
    head_norm_gain,
    mixer_output_weight,
    expert_norm_gain,
    routed_expert_index,
    routed_expert_weight,
    routed_gate_weight,
    routed_up_weight,
    routed_down_weight,
    common_gate_weight,
    common_up_weight,
    common_down_weight,
):
    length, inner = value_projected_input.shape
    heads = step_preactivation.shape[1]
    groups = state_projected_input.shape[1] // STATE
    row_count, width = residual.shape
    sp_size, tp_size = lax.axis_size("sp"), lax.axis_size("tp")
    sp_place = lax.axis_index("sp").astype(jnp.int32).reshape(1)
    tp_place = lax.axis_index("tp").astype(jnp.int32).reshape(1)
    line = sp_size // 2
    top_count = routed_expert_index.shape[1]
    experts_all = routed_gate_weight.shape[0] * sp_size
    dense = (
        line == 4
        and routed_gate_weight.shape[0] == 1
        and 2 * top_count >= experts_all
        and tp_size == 4
    )

    rim_own = jnp.concatenate(
        [a[length - RIM :] for a in (value_projected_input, state_projected_input, readout_projected_input)],
        axis=1,
    )
    rim = lax.ppermute(rim_own, "sp", [(i, i + 1) for i in range(sp_size - 1)])

    if dense:
        def tp_swap(a, k):
            return lax.ppermute(a, "tp", [(i, i ^ k) for i in range(tp_size)])

        shared_gu = jnp.concatenate([common_gate_weight, common_up_weight], axis=1)
        shared_all = [[w, tp_swap(w, 2)] for w in (shared_gu, common_down_weight)]
        shared_all = [pair + [tp_swap(w, 1) for w in pair] for pair in shared_all]
        dense_weight = jnp.sum(
            jnp.where(
                routed_expert_index[:, :, None] == jnp.arange(experts_all, dtype=jnp.int32),
                routed_expert_weight[:, :, None],
                0.0,
            ),
            axis=1,
        )

    rates = head_log_decay_rates.reshape(1, heads)
    direct = head_direct_weight.reshape(1, heads)
    gain = head_norm_gain.reshape(1, inner)
    group_width = inner // groups
    per = groups * (group_width // LANES) * STATE // sp_size
    ext_shapes = [pltpu.VMEM((RIM + BLOCK, w), F32) for w in (group_width, STATE)]
    common_outs = [
        ((BLOCK, inner), BF16),
        ((BLOCK, groups * STATE), BF16),
        ((BLOCK, heads), F32),
        ((BLOCK, heads), F32),
    ]
    front_args = (
        value_projected_input,
        state_projected_input,
        step_preactivation,
        position_decay_extra,
        rates,
        value_conv_kernel,
        state_conv_kernel,
    )
    front_flops = 200_000_000
    val1, b1, dt1, cum1, f1, dec1 = call(
        functools.partial(front_kernel, 1, groups),
        common_outs + [((groups * STATE, group_width), F32), ((8, inner), F32)],
        *front_args,
        flops=front_flops,
        scratch=ext_shapes,
    )
    val0, b0, dt0, cum0, f0, chunks = call(
        functools.partial(front_kernel, 0, groups),
        common_outs
        + [((groups * STATE, group_width), BF16), ((sp_size, per + PAD_ROWS, LANES), BF16)],
        *front_args,
        rim,
        f1,
        dec1,
        flops=front_flops,
        scratch=ext_shapes,
    )
    arrived = lax.all_to_all(chunks, "sp", split_axis=0, concat_axis=0, tiled=True)
    (prefixes,) = call(scan_kernel, [((sp_size, per, LANES), BF16)], arrived, flops=1_000_000)
    states = lax.all_to_all(prefixes, "sp", split_axis=0, concat_axis=0, tiled=True)
    states = states.reshape(sp_size * per, LANES)
    y_local, readout, gate, entry_decay = call(
        functools.partial(middle_kernel, groups),
        [
            ((length, inner), F32),
            ((length, groups * STATE), BF16),
            ((length, inner), BF16),
            ((length, inner), BF16),
        ],
        readout_projected_input,
        rim,
        readout_conv_kernel,
        output_gate_projected,
        direct,
        val0,
        val1,
        b0,
        b1,
        dt0,
        dt1,
        cum0,
        cum1,
        f0,
        flops=400_000_000,
        scratch=[pltpu.VMEM((RIM + BLOCK, STATE), F32)],
    )
    w_chunks = 4
    parts = call(
        functools.partial(mixer_kernel, groups, tp_size),
        [((row_count, width), BF16)] * tp_size,
        tp_place,
        states,
        y_local,
        readout,
        gate,
        entry_decay,
        gain,
        mixer_output_weight,
        flops=2 * length * inner * width,
        scratch=[
            pltpu.VMEM((length, inner), BF16),
            pltpu.VMEM((length, width), BF16),
            pltpu.VMEM((w_chunks, inner, width // w_chunks), BF16),
            pltpu.SemaphoreType.DMA((w_chunks,)),
        ],
        specs=[SMEM] + [None] * 6 + [HBM],
    )
    parts = [parts[0]] + [
        lax.ppermute(parts[k], "tp", [(i, i ^ k) for i in range(tp_size)])
        for k in sorted(range(1, tp_size), reverse=True)
    ]
    stream, normed_rows = call(
        stream_kernel,
        [((row_count, width), BF16)] * 2,
        residual,
        expert_norm_gain.reshape(1, width),
        *parts,
        flops=1_000_000,
    )
    if not dense:
        return sparse_experts(
            stream,
            normed_rows,
            routed_expert_index,
            routed_expert_weight,
            routed_gate_weight,
            routed_up_weight,
            routed_down_weight,
            common_gate_weight,
            common_up_weight,
            common_down_weight,
        )

    up_one = line_pairs(line, [(z, z + 1) for z in range(line)])
    down_one = line_pairs(line, [(z, z - 1) for z in range(line)])
    ends = line_pairs(line, [(0, line - 1), (line - 1, 0)])
    up_far = line_pairs(line, [(1, 2), (2, 3)])
    down_far = line_pairs(line, [(1, 0), (2, 1)])
    back_up = line_pairs(line, [(0, 1), (1, 2)])
    back_down = line_pairs(line, [(2, 1), (3, 2)])

    def spread(a):
        below = lax.ppermute(a, "sp", up_one)
        above = lax.ppermute(a, "sp", down_one)
        far = lax.ppermute(a, "sp", ends)
        return below, above, far, lax.ppermute(below, "sp", up_far), lax.ppermute(above, "sp", down_far)

    tables = spread(dense_weight)
    half = routed_gate_weight.shape[2] // 2
    begin = (tp_place[0] & 1) * half
    gu_half = jnp.concatenate(
        [lax.dynamic_slice_in_dim(w[0], begin, half, 1) for w in (routed_gate_weight, routed_up_weight)],
        axis=1,
    )
    d_half = lax.dynamic_slice_in_dim(routed_down_weight[0], begin, half, 0)
    gu_half, d_half, states_tie = lax.optimization_barrier((gu_half, d_half, states[0:8]))
    other = [(i, i ^ 1) for i in range(sp_size)]
    gu_a = lax.ppermute(gu_half, "sp", other)
    d_a = lax.ppermute(d_half, "sp", other)
    gu_b, d_b = tp_swap(gu_a, 1), tp_swap(d_a, 1)

    below, above, far, below2, above2 = spread(normed_rows)
    (base,) = call(
        shared_kernel,
        [((row_count, width), F32)],
        normed_rows,
        stream,
        *shared_all[0],
        *shared_all[1],
        flops=400_000_000,
    )
    expert_weights = (routed_gate_weight, routed_up_weight, routed_down_weight, gu_a, gu_b, d_a, d_b)
    block_out = ((row_count, width), BF16)
    p_own, p_below, p_above = call(
        functools.partial(expert_kernel, (1, 1, 1)),
        [block_out] * 3,
        sp_place,
        normed_rows,
        below,
        above,
        dense_weight,
        tables[0],
        tables[1],
        *expert_weights,
        flops=1_200_000_000,
        specs=[SMEM] + [None] * 13,
    )
    p_two, p_far = call(
        functools.partial(expert_kernel, (2, 1)),
        [block_out] * 2,
        sp_place,
        below2,
        above2,
        far,
        tables[3],
        tables[4],
        tables[2],
        *expert_weights,
        flops=800_000_000,
        specs=[SMEM] + [None] * 13,
    )
    from_below = lax.ppermute(p_two, "sp", back_up)
    from_above = lax.ppermute(p_two, "sp", back_down)
    r_far = lax.ppermute(p_far, "sp", ends)
    to_above = (p_above.astype(F32) + from_below.astype(F32)).astype(BF16)
    to_below = (p_below.astype(F32) + from_above.astype(F32)).astype(BF16)
    r_below = lax.ppermute(to_above, "sp", up_one)
    r_above = lax.ppermute(to_below, "sp", down_one)
    total = base + p_own.astype(F32) + r_far.astype(F32) + r_below.astype(F32) + r_above.astype(F32)
    return total.astype(BF16)


def solution(mesh):
    placed = (
        P(("sp", "tp"), None),
        P("sp", "tp"),
        P("sp", "tp"),
        P("sp", "tp"),
        P("sp", "tp"),
        P("sp", "tp"),
        P("sp", "tp"),
        P(None, "tp"),
        P(None, "tp"),
        P(None, "tp"),
        P("tp"),
        P("tp"),
        P("tp"),
        P("tp", None),
        P(),
        P(("sp", "tp"), None),
        P(("sp", "tp"), None),
        P("sp", None, None),
        P("sp", None, None),
        P("sp", None, None),
        P(None, "tp"),
        P(None, "tp"),
        P(None, "tp"),
    )
    return jax.shard_map(
        shards, mesh=mesh, in_specs=placed, out_specs=P(("sp", "tp"), None), check_vma=False
    )
```
